32 devices in a mesh: ep: 8 (over z, x), tp: 4 (over y, core).
Axes of the slice: x: 2, y: 2, z: 4, core: 2. Of those that a mesh axis runs over, the one named last changes fastest.
Arguments:
- tokens: bfloat16 [192, 4096], P('ep'), may hold values from -6 to 6
- norm_gain: bfloat16 [4096], replicated, may hold values from 0.099609375 to 1.8984375
- w_query: bfloat16 [4096, 1024], P('ep', 'tp'), may hold values from -0.09375 to 0.09375
- w_key: bfloat16 [4096, 1024], P('ep', 'tp'), may hold values from -0.09375 to 0.09375
- w_value: bfloat16 [4096, 2048], P('ep', 'tp'), may hold values from -0.09375 to 0.09375
- w_rgate: bfloat16 [4096, 2048], P('ep', 'tp'), may hold values from -0.09375 to 0.09375
- w_decay: bfloat16 [4096, 1024], P('ep', 'tp'), may hold values from -0.375 to 0.375
- decay_shift: float32 [192, 1024], P('ep', 'tp'), may hold values from -2 to 0
- state: float32 [192, 8, 128, 256], P('ep', 'tp'), may hold values from -6 to 6
- head_gain: bfloat16 [2048], P('tp'), may hold values from 0.099609375 to 1.8984375
- w_out: bfloat16 [2048, 4096], P('tp', 'ep'), may hold values from -0.125 to 0.125
- ffn_gain: bfloat16 [4096], replicated, may hold values from 0.099609375 to 1.8984375
- w_gate: bfloat16 [8, 4096, 1024], P('ep', None, 'tp'), may hold values from -0.21875 to 0.21875
- w_lin: bfloat16 [8, 4096, 1024], P('ep', None, 'tp'), may hold values from -0.21875 to 0.21875
- w_down: bfloat16 [8, 1024, 4096], P('ep', 'tp'), may hold values from -0.046875 to 0.046875
- expert_ids: int32 [192, 4], P('ep'), may hold values from 0 to 7, all different within a row; in each aligned block of 24 rows (0 to 23, 24 to 47, ...) at most 24 rows name the same one
- route_weight: float32 [192, 4], P('ep'), may hold values from 0.2 to 1
Outputs:
- result: bfloat16 [192, 4096], P('ep')
The draws below stay inside these ranges and needn't reach their ends.
Inputs may be any that keep to these rules, and one draw needn't show every extreme that they name: `expert_ids`: each row names 4 different experts; among the rows of one index of ep no expert is named more than 24 times, a bound that some block reaches.
All inputs are finite; a program needn't handle non-finite values.
Results may differ from the reference program's by a relative error of at most 0.022.
Values may be sent and summed in bfloat16 or wider, within the bound.
A program may use at most 128 MiB of HBM per device.

```python
import math
import jax
import jax.numpy as jnp
import numpy as np
from jax import lax

D = 4096
HEADS = 8
HK = 128
HV = 256
DK = 1024
DV = 2048
DE = 1024
TOP_K = 4
EXPERTS = 8
SEQ_DEV = 24
SEQS = 192
CAP = 24
N_EP = 8
N_TP = 4


def steps_of(stream_key, shape, shards, smallest, largest):
    def one(axis_at, shards_of):
        steps = jax.random.uniform(jax.random.fold_in(jax.random.fold_in(stream_key, 6), axis_at), (shards_of,), jnp.float32, smallest / len(shards), largest / len(shards))
        return jnp.repeat(jnp.exp(steps), shape[axis_at] // shards_of).reshape((-1,) + (1,) * (len(shape) - axis_at - 1))

    level = one(*shards[0])
    for cut in shards[1:]:
        level = level * one(*cut)
    return level


def routed_block(key, own, number, rows, number_of, top, reach, skew):
    ranking = jax.random.permutation(key, number_of)
    crowded, usual = load_shares(number_of, rows * top, reach, skew, True), load_shares(number_of, rows * top, reach, skew, False)
    places = jnp.arange(number_of)

    def named(lengths, offset_by):
        used = int((lengths > 0).sum())
        fixed = max(1, used // 4)
        moved = fixed + (places - fixed + offset_by * (used - fixed)) % max(1, number_of - fixed)
        return jnp.zeros((number_of,), jnp.int32).at[ranking[jnp.where(places < fixed, places, moved)]].set(jnp.asarray(lengths, jnp.int32))

    lengths = jnp.where(number % 4 == 0, named(crowded, number // 4), named(usual, number - number // 4 - 1))
    mixed = jax.random.permutation(jax.random.fold_in(own, 3), number_of)
    giver, receiver = mixed[0:number_of // 2 * 2:2], mixed[1:number_of // 2 * 2:2]
    room = jnp.minimum(lengths[giver] - 1, reach - lengths[receiver]) // 2
    room = jnp.where((giver == ranking[0]) | (receiver == ranking[0]) | (lengths[receiver] == 0), 0, jnp.maximum(room, 0))
    moved = jax.random.randint(jax.random.fold_in(own, 4), (number_of // 2,), 0, 1 << 20) % (room + 1)
    lengths = lengths.at[giver].add(-moved).at[receiver].add(moved)
    labels = jnp.searchsorted(jnp.cumsum(lengths), jnp.arange(rows * top), side="right").astype(jnp.int32)
    table = labels.reshape(top, rows).T
    table = table[jax.random.permutation(jax.random.fold_in(own, 1), rows)]
    offset_by = jax.random.randint(jax.random.fold_in(own, 2), (rows, 1), 0, top)
    return jnp.take_along_axis(table, (jnp.arange(top)[None, :] + offset_by) % top, axis=1)


def load_shares(count, total, most, slope, full):
    loads = [(1 << 20) // math.isqrt(standing ** slope) + 1 for standing in range(1, count + 1)]
    largest = most if full else min(most, max(-(-total // count), total * loads[0] // sum(loads)))
    least = 1 if total - largest >= count - 1 else 0
    given, rest = [largest] + [least] * (count - 1), total - largest - least * (count - 1)
    while rest > 0:
        candidates = [i for i in range(1, count) if given[i] < largest] or [i for i in range(1, count) if given[i] < most]
        pool, left = sum([loads[i] for i in candidates]), rest
        for i in candidates:
            addition = min(most - given[i], max(1, left * loads[i] // pool), rest)
            given[i] = given[i] + addition
            rest = rest - addition
    return np.array(given)


def centred(own_key, shape, deviation, most, shards=(), held_as=jnp.bfloat16):
    factor_of = steps_of(own_key, shape, shards, -0.22, 0.18) if shards else 1.0
    result = jax.random.normal(own_key, shape, jnp.float32) * deviation * factor_of
    return jnp.minimum(jnp.maximum(result, -most), most).astype(held_as)


def setup_inputs(seed: int = 0) -> dict:
    seeds = jax.random.split(jax.random.key(seed), 18)
    tokens = centred(seeds[0], (SEQS, D), 1.0, 6.0, ((0, 8),))
    norm_gain = jnp.clip(1.0 + 0.18 * jax.random.normal(seeds[1], (D,), jnp.float32), 0.099609375, 1.8984375).astype(jnp.bfloat16)
    w_query = centred(seeds[2], (D, DK), D ** -0.5, 0.09375, ((0, 8), (1, 4)))
    w_key = centred(seeds[3], (D, DK), D ** -0.5, 0.09375, ((0, 8), (1, 4)))
    w_value = centred(seeds[4], (D, DV), D ** -0.5, 0.09375, ((0, 8), (1, 4)))
    w_rgate = centred(seeds[5], (D, DV), D ** -0.5, 0.09375, ((0, 8), (1, 4)))
    w_decay = centred(seeds[6], (D, DK), (D // 16) ** -0.5, 0.375, ((0, 8), (1, 4)))
    decay_shift = jnp.clip(-2.0 + 2.0 * jax.random.uniform(seeds[7], (SEQS, DK), jnp.float32) ** steps_of(seeds[7], (SEQS, DK), ((0, 8), (1, 4)), -0.2, 0.2), -2.0, 0.0)
    state = centred(seeds[8], (SEQS, HEADS, HK, HV), 1.0, 6.0, ((0, 8), (1, 4)), jnp.float32)
    head_gain = jnp.clip(1.0 + 0.18 * jax.random.normal(seeds[9], (DV,), jnp.float32), 0.099609375, 1.8984375).astype(jnp.bfloat16)
    w_out = centred(seeds[10], (DV, D), DV ** -0.5, 0.125, ((0, 4), (1, 8)))
    ffn_gain = jnp.clip(1.0 + 0.18 * jax.random.normal(seeds[11], (D,), jnp.float32), 0.099609375, 1.8984375).astype(jnp.bfloat16)
    w_gate = centred(seeds[12], (EXPERTS, D, DE), (D // 6) ** -0.5, 0.21875, ((0, 8), (2, 4)))
    w_lin = centred(seeds[13], (EXPERTS, D, DE), (D // 6) ** -0.5, 0.21875, ((0, 8), (2, 4)))
    w_down = centred(seeds[14], (EXPERTS, DE, D), (DE * 16) ** -0.5, 0.046875, ((0, 8), (1, 4)))
    expert_ids_keys = jax.random.split(jax.random.fold_in(seeds[15], 1), SEQS // SEQ_DEV)
    expert_ids_turns = jax.random.permutation(jax.random.fold_in(seeds[15], 3), SEQS // SEQ_DEV)
    expert_ids = jax.vmap(lambda own, number: routed_block(jax.random.fold_in(seeds[15], 2), own, number, SEQ_DEV, EXPERTS, TOP_K, CAP, 2))(expert_ids_keys, expert_ids_turns).reshape((SEQS, TOP_K))
    route_weight = jnp.clip(0.2 + 0.8 * jax.random.uniform(seeds[16], (SEQS, TOP_K), jnp.float32) ** steps_of(seeds[16], (SEQS, TOP_K), ((0, 8),), -0.2, 0.2), 0.2, 1.0)
    return {"tokens": tokens, "norm_gain": norm_gain, "w_query": w_query, "w_key": w_key, "w_value": w_value, "w_rgate": w_rgate, "w_decay": w_decay, "decay_shift": decay_shift, "state": state, "head_gain": head_gain, "w_out": w_out, "ffn_gain": ffn_gain, "w_gate": w_gate, "w_lin": w_lin, "w_down": w_down, "expert_ids": expert_ids, "route_weight": route_weight}


eps = 1e-06
tau = 16.0
limit = 7.0
glu_alpha = 1.702

def rms_scale(values, gain):
    meansq = lax.optimization_barrier(jnp.mean(values * values, axis=-1, keepdims=True))
    return values * lax.rsqrt(meansq + eps) * gain

def expert_apply(rows, gate_w, lin_w, down_w):
    gate = jnp.dot(rows, gate_w, preferred_element_type=jnp.float32)
    linear = jnp.dot(rows, lin_w, preferred_element_type=jnp.float32)
    gate = jnp.minimum(gate, limit)
    linear = jnp.clip(linear, -limit, limit)
    act = (gate * jax.nn.sigmoid(glu_alpha * gate) * (linear + 1.0)).astype(jnp.bfloat16)
    span = act.shape[1] // N_TP
    total = jnp.zeros((rows.shape[0], down_w.shape[1]), jnp.float32)
    for portion in range(N_TP):
        piece = jnp.dot(act[:, portion * span:(portion + 1) * span], down_w[portion * span:(portion + 1) * span], preferred_element_type=jnp.float32)
        total = total + lax.optimization_barrier(piece.astype(jnp.bfloat16)).astype(jnp.float32)
    return total.astype(jnp.bfloat16)

def reference(tokens, norm_gain, w_query, w_key, w_value, w_rgate, w_decay, decay_shift, state, head_gain, w_out, ffn_gain, w_gate, w_lin, w_down, expert_ids, route_weight):
    seqs = tokens.shape[0]
    width = tokens.shape[1]
    heads = state.shape[1]
    key_dim = state.shape[2]
    val_dim = state.shape[3]
    inputs = tokens.astype(jnp.float32)
    normed = rms_scale(inputs, norm_gain.astype(jnp.float32)).astype(jnp.bfloat16)
    queries = jnp.dot(normed, w_query, preferred_element_type=jnp.float32).astype(jnp.bfloat16)
    keys_new = jnp.dot(normed, w_key, preferred_element_type=jnp.float32).astype(jnp.bfloat16)
    values_new = jnp.dot(normed, w_value, preferred_element_type=jnp.float32).astype(jnp.bfloat16)
    rgates = jnp.dot(normed, w_rgate, preferred_element_type=jnp.float32).astype(jnp.bfloat16)
    decay_pre = jnp.dot(normed, w_decay, preferred_element_type=jnp.float32).astype(jnp.bfloat16)
    log_decay = jax.nn.log_sigmoid(decay_pre.astype(jnp.float32)) / tau + decay_shift
    q_rows = queries.astype(jnp.float32).reshape(seqs, heads, key_dim) * key_dim ** (-0.5)
    k_rows = keys_new.astype(jnp.float32).reshape(seqs, heads, key_dim)
    v_rows = values_new.astype(jnp.float32).reshape(seqs, heads, val_dim)
    new_state = jnp.exp(log_decay.reshape(seqs, heads, key_dim))[..., None] * state + k_rows[..., None] * v_rows[:, :, None, :]
    read = jnp.einsum('shk,shkv->shv', q_rows, new_state, precision=lax.Precision.HIGHEST)
    gated = rms_scale(read, head_gain.astype(jnp.float32).reshape(heads, val_dim))
    gated = gated * jax.nn.silu(rgates.astype(jnp.float32).reshape(seqs, heads, val_dim))
    gated = gated.reshape(seqs, heads * val_dim).astype(jnp.bfloat16)
    span = heads * val_dim // N_TP
    mixed = jnp.zeros((seqs, width), jnp.float32)
    for portion in range(N_TP):
        piece = jnp.dot(gated[:, portion * span:(portion + 1) * span], w_out[portion * span:(portion + 1) * span], preferred_element_type=jnp.float32)
        mixed = mixed + lax.optimization_barrier(piece.astype(jnp.bfloat16)).astype(jnp.float32)
    mixed = mixed.astype(jnp.bfloat16)
    stream = inputs + mixed.astype(jnp.float32)
    ffn_in = rms_scale(stream, ffn_gain.astype(jnp.float32)).astype(jnp.bfloat16)
    experts = w_gate.shape[0]
    top = expert_ids.shape[1]
    slots = N_EP * CAP
    flat_ids = expert_ids.reshape(-1).astype(jnp.int32)
    onehot = (flat_ids[:, None] == jnp.arange(experts, dtype=jnp.int32)[None, :]).astype(jnp.int32)
    rank = lax.optimization_barrier(jnp.sum((jnp.cumsum(onehot, axis=0) - onehot) * onehot, axis=1)).astype(jnp.int32)
    dest = (flat_ids * slots + rank).astype(jnp.int32)
    owner = jnp.repeat(jnp.arange(seqs, dtype=jnp.int32), top)
    table = jnp.full((experts * slots,), seqs, jnp.int32).at[dest].set(owner)
    padded = jnp.concatenate([ffn_in, jnp.zeros((1, width), jnp.bfloat16)], axis=0)

    def one_expert(index):
        picks = lax.dynamic_slice_in_dim(table, (index * slots).astype(jnp.int32), slots)
        return expert_apply(padded[picks], w_gate[index], w_lin[index], w_down[index])
    outputs = lax.map(one_expert, jnp.arange(experts, dtype=jnp.int32))
    picked = outputs.reshape(experts * slots, width)[dest].astype(jnp.float32).reshape(seqs, top, width)
    routed = lax.optimization_barrier(jnp.sum(picked * route_weight[..., None], axis=1))
    return (stream + routed).astype(jnp.bfloat16)
```

```python
import functools

import jax
import jax.numpy as jnp
from jax import lax
from jax.experimental import pallas as pl
from jax.experimental.pallas import tpu as pltpu
from jax.sharding import PartitionSpec as P

eps = 1e-06
tau = 16.0
limit = 7.0
glu_alpha = 1.702


def rms_scale(values, gain):
    meansq = jnp.mean(values * values, axis=-1, keepdims=True)
    return values * lax.rsqrt(meansq + eps) * gain


def activate(gate, linear):
    gate = jnp.minimum(gate, limit)
    linear = jnp.clip(linear, -limit, limit)
    return (gate * jax.nn.sigmoid(glu_alpha * gate) * (linear + 1.0)).astype(jnp.bfloat16)


MESH = pl.DeviceIdType.MESH


def greet(partners):
    barrier = pltpu.get_barrier_semaphore()
    for partner in partners:
        pl.semaphore_signal(barrier, inc=1, device_id=partner, device_id_type=MESH)
    pl.semaphore_wait(barrier, len(partners))


def remote(src, dst, send, recv, partner):
    return pltpu.make_async_remote_copy(
        src_ref=src,
        dst_ref=dst,
        send_sem=send,
        recv_sem=recv,
        device_id=partner,
        device_id_type=MESH,
    )


def others(axis, n):
    me = lax.axis_index(axis)
    return [{axis: lax.rem(me + k, n)} for k in range(1, n)]


def across(axis, distance):
    me = lax.axis_index(axis)
    digit = lax.rem(me // distance, 2)
    return {axis: me + distance - 2 * distance * digit}, digit


def digits_of(n):
    values = []
    while n > 1:
        n //= 2
        values.append(n)
    return values


def comm_call(kernel, ins, out_shape, scratch, number):
    return pl.pallas_call(
        kernel,
        out_shape=out_shape,
        in_specs=[pl.BlockSpec(memory_space=pltpu.VMEM)] * len(ins),
        out_specs=jax.tree.map(lambda _: pl.BlockSpec(memory_space=pltpu.VMEM), out_shape),
        scratch_shapes=scratch,
        compiler_params=pltpu.CompilerParams(
            collective_id=number, has_side_effects=True, vmem_limit_bytes=32 * 1024 * 1024
        ),
    )(*ins)


def token_kernel(n, tok_ref, wt_ref, rows_ref, all_wt_ref, send, recv, send_w, recv_w, local):
    me = lax.axis_index("ep")
    span = rows_ref.shape[2]
    partners = others("ep", n)
    greet(partners)
    copies = []
    for k, partner in enumerate(partners):
        cols = pl.ds(pl.multiple_of(partner["ep"] * span, span), span)
        copies.append(
            remote(tok_ref.at[:, cols], rows_ref.at[me], send.at[k], recv.at[k], partner)
        )
        copies.append(remote(wt_ref, all_wt_ref.at[me], send_w.at[k], recv_w.at[k], partner))
    for copy in copies:
        copy.start()
    own = pl.ds(pl.multiple_of(me * span, span), span)
    keep = pltpu.make_async_copy(tok_ref.at[:, own], rows_ref.at[me], local.at[0])
    keep_w = pltpu.make_async_copy(wt_ref, all_wt_ref.at[me], local.at[1])
    keep.start()
    keep_w.start()
    keep.wait()
    keep_w.wait()
    for copy in copies:
        copy.wait()


def spread_tokens(tokens, weights, n):
    rows, width = tokens.shape
    dma = pltpu.SemaphoreType.DMA
    return comm_call(
        functools.partial(token_kernel, n),
        (tokens, weights),
        (
            jax.ShapeDtypeStruct((n, rows, width // n), tokens.dtype),
            jax.ShapeDtypeStruct((n,) + weights.shape, weights.dtype),
        ),
        [dma((n - 1,)), dma((n - 1,)), dma((n - 1,)), dma((n - 1,)), dma((2,))],
        1,
    )


def swap_kernel(n, every, x_ref, out_ref, send, recv, local):
    me = lax.axis_index("ep")
    partners = others("ep", n)
    greet(partners)
    copies = []
    for k, partner in enumerate(partners):
        src = x_ref if every else x_ref.at[partner["ep"]]
        copies.append(remote(src, out_ref.at[me], send.at[k], recv.at[k], partner))
    for copy in copies:
        copy.start()
    keep = pltpu.make_async_copy(x_ref if every else x_ref.at[me], out_ref.at[me], local)
    keep.start()
    keep.wait()
    for copy in copies:
        copy.wait()


def swap(x, n, every, number):
    dma = pltpu.SemaphoreType.DMA
    return comm_call(
        functools.partial(swap_kernel, n, every),
        (x,),
        jax.ShapeDtypeStruct(((n,) + x.shape) if every else x.shape, x.dtype),
        [dma((n - 1,)), dma((n - 1,)), dma],
        number,
    )


def stream_kernel(n_ep, n_tp, x_ref, tok_ref, out_ref, land, send_t, recv_t, send, recv):
    me = lax.axis_index("tp")
    partners = others("tp", n_tp)
    stages = [across("ep", d) for d in digits_of(n_ep)]
    greet(partners + [partner for partner, _ in stages])
    stages += [across("tp", d) for d in digits_of(n_tp)]
    copies = [
        remote(x_ref.at[partner["tp"]], land.at[k], send_t.at[k], recv_t.at[k], partner)
        for k, partner in enumerate(partners)
    ]
    for copy in copies:
        copy.start()
    for copy in copies:
        copy.wait()
    place = sum(digit * 2**k for k, (_, digit) in enumerate(stages))
    total = x_ref[me].astype(jnp.float32)
    for k in range(n_tp - 1):
        total = total + land[k].astype(jnp.float32)
    mixed = total.astype(jnp.bfloat16).astype(jnp.float32)
    out_ref[place] = (tok_ref[...].astype(jnp.float32) + mixed).astype(out_ref.dtype)
    for k, (partner, _) in enumerate(stages):
        held = out_ref.at[pl.ds((place // 2**k) * 2**k, 2**k)]
        copy = remote(held, held, send.at[k], recv.at[k], partner)
        copy.start()
        copy.wait()


def gather_stream(partial_value, tok, n_ep, n_tp, number):
    dma = pltpu.SemaphoreType.DMA
    depth = len(digits_of(n_ep)) + len(digits_of(n_tp))
    return comm_call(
        functools.partial(stream_kernel, n_ep, n_tp),
        (partial_value, tok),
        jax.ShapeDtypeStruct((n_ep * n_tp,) + tok.shape, jnp.bfloat16),
        [
            pltpu.VMEM((n_tp - 1,) + tok.shape, jnp.bfloat16),
            dma((n_tp - 1,)),
            dma((n_tp - 1,)),
            dma((depth,)),
            dma((depth,)),
        ],
        number,
    )


def combine_kernel(n_ep, n_tp, x_ref, out_ref, work, land, send, recv, send_t, recv_t, local):
    me = lax.axis_index("tp")
    partners = others("tp", n_tp)
    ep_stages = [across("ep", d) for d in reversed(digits_of(n_ep))]
    greet(partners + [partner for partner, _ in ep_stages])
    stages = [across("tp", d) for d in reversed(digits_of(n_tp))] + ep_stages
    source, size, at = x_ref, n_ep * n_tp, 0
    for k, (partner, digit) in enumerate(stages):
        size //= 2
        copy = remote(
            source.at[pl.ds((1 - digit) * size, size)],
            land.at[pl.ds(at, size)],
            send.at[k],
            recv.at[k],
            partner,
        )
        copy.start()
        copy.wait()

        def add(j, _, source=source, size=size, at=at, digit=digit):
            both = source[digit * size + j].astype(jnp.float32) + land[at + j].astype(jnp.float32)
            work[at + j] = both.astype(work.dtype)
            return 0

        lax.fori_loop(0, size, add, 0)
        source, at = work.at[pl.ds(at, size)], at + size
    copies = [
        remote(source.at[0], out_ref.at[me], send_t.at[k], recv_t.at[k], partner)
        for k, partner in enumerate(partners)
    ]
    for copy in copies:
        copy.start()
    keep = pltpu.make_async_copy(source.at[0], out_ref.at[me], local)
    keep.start()
    keep.wait()
    for copy in copies:
        copy.wait()


def combine(blocks, n_ep, n_tp, number):
    dma = pltpu.SemaphoreType.DMA
    depth = len(digits_of(n_ep)) + len(digits_of(n_tp))
    block = blocks.shape[1:]
    return comm_call(
        functools.partial(combine_kernel, n_ep, n_tp),
        (blocks,),
        jax.ShapeDtypeStruct((n_tp,) + block, jnp.bfloat16),
        [
            pltpu.VMEM((n_ep * n_tp - 1,) + block, jnp.bfloat16),
            pltpu.VMEM((n_ep * n_tp - 1,) + block, jnp.bfloat16),
            dma((depth,)),
            dma((depth,)),
            dma((n_tp - 1,)),
            dma((n_tp - 1,)),
            dma,
        ],
        number,
    )


def folded(blocks):
    lead, (rows, cols) = blocks.shape[:-2], blocks.shape[-2:]
    halves = jnp.swapaxes(blocks.reshape(lead + (rows, 2, cols // 2)), -3, -2)
    return halves.reshape(lead + (2 * rows, cols // 2))


def unfolded(blocks):
    lead, (rows, cols) = blocks.shape[:-2], blocks.shape[-2:]
    halves = jnp.swapaxes(blocks.reshape(lead + (2, rows // 2, cols)), -3, -2)
    return halves.reshape(lead + (rows // 2, 2 * cols))


def on_device_dense(
    tokens,
    norm_gain,
    w_query,
    w_key,
    w_value,
    w_rgate,
    w_decay,
    decay_shift,
    state,
    head_gain,
    w_out,
    ffn_gain,
    w_gate,
    w_lin,
    w_down,
    expert_ids,
    route_weight,
):
    n_ep, n_tp = lax.axis_size("ep"), lax.axis_size("tp")
    my_ep, my_tp = lax.axis_index("ep"), lax.axis_index("tp")
    seq_dev, width = tokens.shape
    heads_dev, key_dim, val_dim = state.shape[1:]
    key_cols = w_query.shape[1]
    val_cols = w_value.shape[1]
    exp_dev = w_gate.shape[0]
    experts = exp_dev * n_ep
    seqs = seq_dev * n_ep
    span = width // n_ep
    lanes = -(-experts // 128) * 128
    named = expert_ids[:, :, None] == jnp.arange(lanes, dtype=jnp.int32)
    weights = jnp.sum(jnp.where(named, route_weight[:, :, None], 0.0), axis=1)

    rows, all_weights = spread_tokens(tokens, weights, n_ep)
    rows = rows.reshape(seqs, span)
    gain = lax.dynamic_slice_in_dim(norm_gain, my_ep * span, span).astype(jnp.float32)
    scaled = (rows.astype(jnp.float32) * gain).astype(jnp.bfloat16)
    parts = [
        jnp.dot(scaled, w, preferred_element_type=jnp.float32).astype(jnp.bfloat16)
        for w in (w_query, w_key, w_decay, w_value, w_rgate)
    ]
    joined = jnp.concatenate(parts, axis=1)
    sums = swap(folded(joined.reshape(n_ep, seq_dev, -1)), n_ep, False, 2)
    inputs = tokens.astype(jnp.float32)
    inverse = lax.rsqrt(jnp.mean(inputs * inputs, axis=-1, keepdims=True) + eps)
    projected = unfolded(jnp.sum(sums.astype(jnp.float32), axis=0)) * inverse

    q_rows = projected[:, :key_cols].reshape(seq_dev, heads_dev, key_dim) * key_dim ** (-0.5)
    k_rows = projected[:, key_cols : 2 * key_cols].reshape(seq_dev, heads_dev, key_dim)
    decay_pre = projected[:, 2 * key_cols : 3 * key_cols]
    v_rows = projected[:, 3 * key_cols : 3 * key_cols + val_cols].reshape(
        seq_dev, heads_dev, val_dim
    )
    rgates = projected[:, 3 * key_cols + val_cols :].reshape(seq_dev, heads_dev, val_dim)
    log_decay = jax.nn.log_sigmoid(decay_pre) / tau + decay_shift
    decayed = q_rows * jnp.exp(log_decay.reshape(seq_dev, heads_dev, key_dim))
    read = (
        jnp.sum(decayed[..., None] * state, axis=2)
        + jnp.sum(q_rows * k_rows, axis=-1, keepdims=True) * v_rows
    )
    gated = rms_scale(
        read, head_gain.astype(jnp.float32).reshape(heads_dev, val_dim)
    ) * jax.nn.silu(rgates)
    gated = gated.reshape(seq_dev, heads_dev * val_dim).astype(jnp.bfloat16)

    all_gated = swap(gated, n_ep, True, 3).reshape(seqs, heads_dev * val_dim)
    cols = w_out.shape[1] // n_tp
    partial_value = jnp.dot(all_gated, w_out, preferred_element_type=jnp.float32)
    partial_value = partial_value.astype(jnp.bfloat16).reshape(seqs, n_tp, cols).swapaxes(0, 1)
    own_tokens = lax.dynamic_slice_in_dim(rows, my_tp * cols, cols, axis=1)
    blocks = gather_stream(partial_value, own_tokens, n_ep, n_tp, 4)

    ep_bits, tp_bits = len(digits_of(n_ep)), len(digits_of(n_tp))
    bits = ep_bits + tp_bits
    order = [bits - 1 - k for k in range(bits)]
    stream = blocks.reshape((2,) * bits + (seqs, cols))
    stream = stream.transpose([bits] + order + [bits + 1]).reshape(seqs, width)
    stream = stream.astype(jnp.float32)
    ffn_in = rms_scale(stream, ffn_gain.astype(jnp.float32)).astype(jnp.bfloat16)
    own_weights = lax.dynamic_slice_in_dim(
        all_weights.reshape(seqs, lanes), my_ep * exp_dev, exp_dev, axis=1
    )
    total = 0.0
    for index in range(exp_dev):
        gate = jnp.dot(ffn_in, w_gate[index], preferred_element_type=jnp.float32)
        linear = jnp.dot(ffn_in, w_lin[index], preferred_element_type=jnp.float32)
        act = activate(gate, linear)
        partial_out = jnp.dot(act, w_down[index], preferred_element_type=jnp.float32)
        total = total + partial_out * own_weights[:, index : index + 1]
    total = total.astype(jnp.bfloat16)
    total = total.reshape((2,) * ep_bits + (seq_dev,) + (2,) * tp_bits + (2, width // n_tp // 2))
    tp_at = list(range(ep_bits + 1, ep_bits + 1 + tp_bits))
    moved = tp_at[::-1] + list(range(ep_bits))[::-1]
    last = ep_bits + 1 + tp_bits
    total = total.transpose(moved + [last, ep_bits, last + 1])
    total = total.reshape(n_ep * n_tp, 2 * seq_dev, width // n_tp // 2)
    routed = unfolded(combine(total, n_ep, n_tp, 5)).swapaxes(0, 1).reshape(seq_dev, width)
    own_stream = lax.dynamic_slice_in_dim(stream, my_ep * seq_dev, seq_dev, axis=0)
    return (own_stream + routed.astype(jnp.float32)).astype(jnp.bfloat16)


def is_power(n):
    return n > 1 and n & (n - 1) == 0


def on_device(
    tokens,
    norm_gain,
    w_query,
    w_key,
    w_value,
    w_rgate,
    w_decay,
    decay_shift,
    state,
    head_gain,
    w_out,
    ffn_gain,
    w_gate,
    w_lin,
    w_down,
    expert_ids,
    route_weight,
):
    seq_dev = tokens.shape[0]
    width = tokens.shape[1]
    heads_dev = state.shape[1]
    key_dim = state.shape[2]
    val_dim = state.shape[3]
    key_cols = w_query.shape[1]
    val_cols = w_value.shape[1]
    inputs = tokens.astype(jnp.float32)
    normed = rms_scale(inputs, norm_gain.astype(jnp.float32)).astype(jnp.bfloat16)
    spread = lax.all_to_all(normed, "ep", split_axis=1, concat_axis=0, tiled=True)
    joined = jnp.concatenate((w_query, w_key, w_decay, w_value, w_rgate), axis=1)
    projected = lax.psum_scatter(
        jnp.dot(spread, joined, preferred_element_type=jnp.float32),
        "ep",
        scatter_dimension=0,
        tiled=True,
    )
    projected = projected.astype(jnp.bfloat16).astype(jnp.float32)
    q_rows = projected[:, :key_cols].reshape(seq_dev, heads_dev, key_dim) * key_dim ** (-0.5)
    k_rows = projected[:, key_cols : 2 * key_cols].reshape(seq_dev, heads_dev, key_dim)
    decay_pre = projected[:, 2 * key_cols : 3 * key_cols]
    v_rows = projected[:, 3 * key_cols : 3 * key_cols + val_cols].reshape(
        seq_dev, heads_dev, val_dim
    )
    rgates = projected[:, 3 * key_cols + val_cols :].reshape(seq_dev, heads_dev, val_dim)
    log_decay = jax.nn.log_sigmoid(decay_pre) / tau + decay_shift
    new_state = (
        jnp.exp(log_decay.reshape(seq_dev, heads_dev, key_dim))[..., None] * state
        + k_rows[..., None] * v_rows[:, :, None, :]
    )
    read = jnp.einsum("shk,shkv->shv", q_rows, new_state, precision=lax.Precision.HIGHEST)
    gated = rms_scale(
        read, head_gain.astype(jnp.float32).reshape(heads_dev, val_dim)
    ) * jax.nn.silu(rgates)
    gated = gated.reshape(seq_dev, heads_dev * val_dim).astype(jnp.bfloat16)
    partial_value = jnp.dot(
        lax.all_gather(gated, "ep", axis=0, tiled=True), w_out, preferred_element_type=jnp.float32
    )
    summed = lax.psum(partial_value.astype(jnp.bfloat16), "tp")
    mixed = lax.all_to_all(summed, "ep", split_axis=0, concat_axis=1, tiled=True)
    stream = inputs + mixed.astype(jnp.float32)
    ffn_in = rms_scale(stream, ffn_gain.astype(jnp.float32)).astype(jnp.bfloat16)
    n_ep = lax.axis_size("ep")
    exp_dev = w_gate.shape[0]
    experts = exp_dev * n_ep
    top = expert_ids.shape[1]
    capacity = max(2, 2 * seq_dev * top // experts)
    flat_ids = expert_ids.reshape(-1)
    onehot = (flat_ids[:, None] == jnp.arange(experts, dtype=jnp.int32)[None, :]).astype(jnp.int32)
    rank = jnp.sum((jnp.cumsum(onehot, axis=0) - onehot) * onehot, axis=1)
    slot_of = flat_ids * capacity + rank
    dispatch = (
        jnp.arange(experts * capacity, dtype=jnp.int32)[:, None] == slot_of[None, :]
    ).astype(jnp.bfloat16)
    dispatch = jnp.sum(dispatch.reshape(experts * capacity, seq_dev, top), axis=2)
    outbound = jnp.dot(dispatch, ffn_in, preferred_element_type=jnp.float32).astype(jnp.bfloat16)
    outbound = outbound.reshape(experts, capacity, width)
    arrived = lax.all_to_all(outbound, "ep", split_axis=0, concat_axis=0, tiled=True)
    count = arrived.shape[1]
    rows = arrived.reshape(n_ep, exp_dev, count, width)
    gate = jnp.einsum("secd,edh->sech", rows, w_gate, preferred_element_type=jnp.float32)
    linear = jnp.einsum("secd,edh->sech", rows, w_lin, preferred_element_type=jnp.float32)
    act = activate(gate, linear)
    partial_out = jnp.einsum("sech,ehd->secd", act, w_down, preferred_element_type=jnp.float32)
    summed_out = lax.psum(partial_out.astype(jnp.bfloat16), "tp")
    returned = lax.all_to_all(
        summed_out.reshape(n_ep * exp_dev, count, width),
        "ep",
        split_axis=0,
        concat_axis=0,
        tiled=True,
    )
    picked = (
        returned.reshape(experts * capacity, width)[slot_of]
        .astype(jnp.float32)
        .reshape(seq_dev, top, width)
    )
    routed = jnp.sum(picked * route_weight[..., None], axis=1)
    return (stream + routed).astype(jnp.bfloat16)


def solution(mesh):
    n_ep, n_tp = mesh.shape["ep"], mesh.shape["tp"]

    def chosen(*arrays):
        seq_dev, top = arrays[15].shape
        experts = arrays[12].shape[0] * n_ep
        dense = max(2, 2 * seq_dev * top // experts) >= seq_dev
        whole = arrays[0].shape[1] % (n_ep * n_tp * 128) == 0 and seq_dev % 8 == 0
        if dense and whole and is_power(n_ep) and is_power(n_tp):
            return on_device_dense(*arrays)
        return on_device(*arrays)

    placed = (
        P("ep", None),
        P(),
        P("ep", "tp"),
        P("ep", "tp"),
        P("ep", "tp"),
        P("ep", "tp"),
        P("ep", "tp"),
        P("ep", "tp"),
        P("ep", "tp", None, None),
        P("tp"),
        P("tp", "ep"),
        P(),
        P("ep", None, "tp"),
        P("ep", None, "tp"),
        P("ep", "tp", None),
        P("ep", None),
        P("ep", None),
    )
    return jax.shard_map(
        chosen, mesh=mesh, in_specs=placed, out_specs=P("ep", None), check_vma=False
    )
```

```python
import functools

import jax
import jax.numpy as jnp
from jax import lax
from jax.experimental import pallas as pl
from jax.experimental.pallas import tpu as pltpu
from jax.sharding import PartitionSpec as P

eps = 1e-06
tau = 16.0
limit = 7.0
glu_alpha = 1.702


def rms_scale(values, gain):
    meansq = jnp.mean(values * values, axis=-1, keepdims=True)
    return values * lax.rsqrt(meansq + eps) * gain


def activate(gate, linear):
    gate = jnp.minimum(gate, limit)
    linear = jnp.clip(linear, -limit, limit)
    return (gate * jax.nn.sigmoid(glu_alpha * gate) * (linear + 1.0)).astype(jnp.bfloat16)


MESH = pl.DeviceIdType.MESH


def greet(partners):
    barrier = pltpu.get_barrier_semaphore()
    for partner in partners:
        pl.semaphore_signal(barrier, inc=1, device_id=partner, device_id_type=MESH)
    pl.semaphore_wait(barrier, len(partners))


def remote(src, dst, send, recv, partner):
    return pltpu.make_async_remote_copy(
        src_ref=src,
        dst_ref=dst,
        send_sem=send,
        recv_sem=recv,
        device_id=partner,
        device_id_type=MESH,
    )


def others(axis, n):
    me = lax.axis_index(axis)
    return [{axis: lax.rem(me + k, n)} for k in range(1, n)]


def across(axis, distance):
    me = lax.axis_index(axis)
    digit = lax.rem(me // distance, 2)
    return {axis: me + distance - 2 * distance * digit}, digit


def digits_of(n):
    values = []
    while n > 1:
        n //= 2
        values.append(n)
    return values


def comm_call(kernel, ins, out_shape, scratch, number):
    return pl.pallas_call(
        kernel,
        out_shape=out_shape,
        in_specs=[pl.BlockSpec(memory_space=pltpu.VMEM)] * len(ins),
        out_specs=jax.tree.map(lambda _: pl.BlockSpec(memory_space=pltpu.VMEM), out_shape),
        scratch_shapes=scratch,
        compiler_params=pltpu.CompilerParams(
            collective_id=number, has_side_effects=True, vmem_limit_bytes=32 * 1024 * 1024
        ),
    )(*ins)


def token_kernel(n, tok_ref, wt_ref, rows_ref, all_wt_ref, send, recv, send_w, recv_w, local):
    me = lax.axis_index("ep")
    span = rows_ref.shape[2]
    partners = others("ep", n)
    greet(partners)
    copies = []
    for k, partner in enumerate(partners):
        cols = pl.ds(pl.multiple_of(partner["ep"] * span, span), span)
        copies.append(
            remote(tok_ref.at[:, cols], rows_ref.at[me], send.at[k], recv.at[k], partner)
        )
        copies.append(remote(wt_ref, all_wt_ref.at[me], send_w.at[k], recv_w.at[k], partner))
    for copy in copies:
        copy.start()
    own = pl.ds(pl.multiple_of(me * span, span), span)
    keep = pltpu.make_async_copy(tok_ref.at[:, own], rows_ref.at[me], local.at[0])
    keep_w = pltpu.make_async_copy(wt_ref, all_wt_ref.at[me], local.at[1])
    keep.start()
    keep_w.start()
    keep.wait()
    keep_w.wait()
    for copy in copies:
        copy.wait()


def spread_tokens(tokens, weights, n):
    rows, width = tokens.shape
    dma = pltpu.SemaphoreType.DMA
    return comm_call(
        functools.partial(token_kernel, n),
        (tokens, weights),
        (
            jax.ShapeDtypeStruct((n, rows, width // n), tokens.dtype),
            jax.ShapeDtypeStruct((n,) + weights.shape, weights.dtype),
        ),
        [dma((n - 1,)), dma((n - 1,)), dma((n - 1,)), dma((n - 1,)), dma((2,))],
        1,
    )


def swap_kernel(n, every, x_ref, out_ref, send, recv, local):
    me = lax.axis_index("ep")
    partners = others("ep", n)
    greet(partners)
    copies = []
    for k, partner in enumerate(partners):
        src = x_ref if every else x_ref.at[partner["ep"]]
        copies.append(remote(src, out_ref.at[me], send.at[k], recv.at[k], partner))
    for copy in copies:
        copy.start()
    keep = pltpu.make_async_copy(x_ref if every else x_ref.at[me], out_ref.at[me], local)
    keep.start()
    keep.wait()
    for copy in copies:
        copy.wait()


def swap(x, n, every, number):
    dma = pltpu.SemaphoreType.DMA
    return comm_call(
        functools.partial(swap_kernel, n, every),
        (x,),
        jax.ShapeDtypeStruct(((n,) + x.shape) if every else x.shape, x.dtype),
        [dma((n - 1,)), dma((n - 1,)), dma],
        number,
    )


def axes_of(n_ep, n_tp):
    return [("ep", d) for d in digits_of(n_ep)] + [("tp", d) for d in digits_of(n_tp)]


def orders_of(n_ep, n_tp):
    count = len(axes_of(n_ep, n_tp))
    first = list(range(count))
    second = list(first)
    if count > 2:
        second[-3], second[-2] = second[-2], second[-3]
    return first, second


def stream_kernel(n_ep, n_tp, x_ref, tok_ref, out_ref, land, send_t, recv_t, send, recv):
    me = lax.axis_index("tp")
    partners = others("tp", n_tp)
    axes = axes_of(n_ep, n_tp)
    pairs = [across(*axis) for axis in axes]
    digits = tuple(digit for _, digit in pairs)
    greet(partners + [pair[0] for pair, axis in zip(pairs, axes) if axis[0] == "ep"])
    copies = [
        remote(x_ref.at[partner["tp"]], land.at[k], send_t.at[k], recv_t.at[k], partner)
        for k, partner in enumerate(partners)
    ]
    for copy in copies:
        copy.start()
    for copy in copies:
        copy.wait()
    total = x_ref[me].astype(jnp.float32)
    for k in range(n_tp - 1):
        total = total + land[k].astype(jnp.float32)
    mixed = total.astype(jnp.bfloat16).astype(jnp.float32)
    stream = (tok_ref[...].astype(jnp.float32) + mixed).astype(out_ref.dtype)
    half = stream.shape[0] // 2
    for piece in range(2):
        out_ref[(piece,) + digits] = stream[piece * half : (piece + 1) * half]
    orders = orders_of(n_ep, n_tp)

    def begin(piece, k):
        done = orders[piece][:k]
        place = tuple(slice(None) if i in done else digits[i] for i in range(len(axes)))
        held = out_ref.at[(piece,) + place]
        partner = pairs[orders[piece][k]][0]
        copy = remote(held, held, send.at[piece, k], recv.at[piece, k], partner)
        copy.start()
        return copy

    running = [begin(0, 0), begin(1, 0)]
    for k in range(len(axes)):
        for piece in range(2):
            running[piece].wait()
            if k + 1 < len(axes):
                running[piece] = begin(piece, k + 1)


def gather_stream(partial_value, tok, n_ep, n_tp, number):
    dma = pltpu.SemaphoreType.DMA
    depth = len(axes_of(n_ep, n_tp))
    rows, cols = tok.shape
    return comm_call(
        functools.partial(stream_kernel, n_ep, n_tp),
        (partial_value, tok),
        jax.ShapeDtypeStruct((2,) + (2,) * depth + (rows // 2, cols), jnp.bfloat16),
        [
            pltpu.VMEM((n_tp - 1,) + tok.shape, jnp.bfloat16),
            dma((n_tp - 1,)),
            dma((n_tp - 1,)),
            dma((2, depth)),
            dma((2, depth)),
        ],
        number,
    )


def combine_kernel(n_ep, n_tp, x_ref, out_ref, *scratch):
    axes = axes_of(n_ep, n_tp)
    depth = len(axes)
    lands, works = scratch[:depth], scratch[depth : 2 * depth]
    send, recv, send_t, recv_t, local = scratch[2 * depth :]
    me = lax.axis_index("tp")
    partners = others("tp", n_tp)
    pairs = [across(*axis) for axis in axes]
    greet(partners + [pair[0] for pair, axis in zip(pairs, axes) if axis[0] == "ep"])
    orders = [order[::-1] for order in orders_of(n_ep, n_tp)]

    def piece_of(piece, k, digit):
        done = sorted(orders[piece][:k])
        at = [i for i in range(depth) if i not in done].index(orders[piece][k])
        lead = (slice(None),) * at
        source = x_ref if k == 0 else works[k - 1]
        return source, (piece,) + lead + (digit,), depth - k - 1 - at

    def begin(piece, k):
        partner, digit = pairs[orders[piece][k]]
        source, place, _ = piece_of(piece, k, 1 - digit)
        copy = remote(
            source.at[place], lands[k].at[piece], send.at[piece, k], recv.at[piece, k], partner
        )
        copy.start()
        return copy

    running = [begin(0, 0), begin(1, 0)]
    copies = []
    for k in range(depth):
        for piece in range(2):
            running[piece].wait()
            source, place, _ = piece_of(piece, k, pairs[orders[piece][k]][1])
            at = len(place) - 2
            for block in range(2 ** (depth - k - 1)):
                index = tuple((block >> i) & 1 for i in reversed(range(depth - k - 1)))
                full = (piece,) + index[:at] + (place[-1],) + index[at:]
                both = source[full].astype(jnp.float32)
                both = both + lands[k][(piece,) + index].astype(jnp.float32)
                works[k][(piece,) + index] = both.astype(jnp.bfloat16)
            if k + 1 < depth:
                running[piece] = begin(piece, k + 1)
                continue
            last, goal = works[k].at[piece], out_ref.at[me, piece]
            for j, partner in enumerate(partners):
                copy = remote(last, goal, send_t.at[piece, j], recv_t.at[piece, j], partner)
                copy.start()
                copies.append(copy)
            keep = pltpu.make_async_copy(last, goal, local.at[piece])
            keep.start()
            copies.append(keep)
    for copy in copies:
        copy.wait()


def combine(blocks, n_ep, n_tp, number):
    dma = pltpu.SemaphoreType.DMA
    depth = len(axes_of(n_ep, n_tp))
    block = blocks.shape[-2:]
    halves = [
        pltpu.VMEM((2,) + (2,) * (depth - k - 1) + block, jnp.bfloat16) for k in range(depth)
    ]
    return comm_call(
        functools.partial(combine_kernel, n_ep, n_tp),
        (blocks,),
        jax.ShapeDtypeStruct((n_tp, 2) + block, jnp.bfloat16),
        halves
        + halves
        + [
            dma((2, depth)),
            dma((2, depth)),
            dma((2, n_tp - 1)),
            dma((2, n_tp - 1)),
            dma((2,)),
        ],
        number,
    )


def read_kernel(heads, key_dim, val_dim, tok_ref, sum_ref, shift_ref, state_ref, gain_ref, out_ref):
    inputs = tok_ref[...].astype(jnp.float32)
    inverse = lax.rsqrt(jnp.mean(inputs * inputs, axis=-1, keepdims=True) + eps)
    total = sum_ref[0].astype(jnp.float32)
    for k in range(1, sum_ref.shape[0]):
        total = total + sum_ref[k].astype(jnp.float32)
    projected = total * inverse
    keys, vals = heads * key_dim, heads * val_dim
    for head in range(heads):
        key_at, val_at = head * key_dim, 3 * keys + head * val_dim
        q_rows = projected[:, key_at : key_at + key_dim] * key_dim ** (-0.5)
        k_rows = projected[:, keys + key_at : keys + key_at + key_dim]
        pre = projected[:, 2 * keys + key_at : 2 * keys + key_at + key_dim]
        v_rows = projected[:, val_at : val_at + val_dim]
        rgates = projected[:, val_at + vals : val_at + vals + val_dim]
        log_sig = jnp.minimum(pre, 0.0) - jnp.log1p(jnp.exp(-jnp.abs(pre)))
        log_decay = log_sig / tau + shift_ref[:, key_at : key_at + key_dim]
        decayed = jnp.transpose(q_rows * jnp.exp(log_decay))
        old = [
            jnp.sum(decayed[:, s : s + 1] * state_ref[s, head], axis=0, keepdims=True)
            for s in range(state_ref.shape[0])
        ]
        read = jnp.concatenate(old, axis=0)
        read = read + jnp.sum(q_rows * k_rows, axis=-1, keepdims=True) * v_rows
        cols = slice(head * val_dim, (head + 1) * val_dim)
        gated = rms_scale(read, gain_ref[:, cols].astype(jnp.float32))
        out_ref[:, cols] = (gated * (rgates * jax.nn.sigmoid(rgates))).astype(jnp.bfloat16)


def gated_read(tokens, sums, decay_shift, state, head_gain):
    seq_dev, heads, key_dim, val_dim = state.shape
    tile = 8
    n, _, cols = sums.shape
    return pl.pallas_call(
        functools.partial(read_kernel, heads, key_dim, val_dim),
        grid=(seq_dev // tile,),
        out_shape=jax.ShapeDtypeStruct((seq_dev, heads * val_dim), jnp.bfloat16),
        in_specs=[
            pl.BlockSpec((tile, tokens.shape[1]), lambda i: (i, 0)),
            pl.BlockSpec((n, tile, cols), lambda i: (0, i, 0)),
            pl.BlockSpec((tile, heads * key_dim), lambda i: (i, 0)),
            pl.BlockSpec((tile, heads, key_dim, val_dim), lambda i: (i, 0, 0, 0)),
            pl.BlockSpec((1, heads * val_dim), lambda i: (0, 0)),
        ],
        out_specs=pl.BlockSpec((tile, heads * val_dim), lambda i: (i, 0)),
        compiler_params=pltpu.CompilerParams(vmem_limit_bytes=16 * 1024 * 1024),
    )(tokens, sums, decay_shift, state, head_gain.reshape(1, -1))


def expert_kernel(
    n_ep, n_tp, blocks_ref, gain_ref, gate_ref, lin_ref, down_ref, wt_ref, out_ref, own_ref, ffn
):
    pieces, count, rows, cols = blocks_ref.shape
    seqs, width = ffn.shape
    seq_dev = seqs // n_ep
    me = lax.axis_index("ep")
    per_piece = n_ep // pieces
    first = pl.multiple_of(lax.rem(me, per_piece) * seq_dev, 8)
    for j in range(count):
        at = slice(j * cols, (j + 1) * cols)
        own_ref[:, at] = blocks_ref[me // per_piece, j, pl.ds(first, seq_dev), :]
    for piece in range(pieces):
        square = jnp.zeros((rows, cols), jnp.float32)
        for j in range(count):
            block = blocks_ref[piece, j].astype(jnp.float32)
            square = square + block * block
        inverse = lax.rsqrt(jnp.sum(square, axis=-1, keepdims=True) / width + eps)
        for j in range(count):
            at = slice(j * cols, (j + 1) * cols)
            scaled = blocks_ref[piece, j].astype(jnp.float32) * inverse
            scaled = scaled * gain_ref[:, at].astype(jnp.float32)
            ffn[piece * rows : (piece + 1) * rows, at] = scaled.astype(jnp.bfloat16)
    acts = []
    for index in range(gate_ref.shape[0]):
        gate = jnp.dot(ffn[...], gate_ref[index], preferred_element_type=jnp.float32)
        linear = jnp.dot(ffn[...], lin_ref[index], preferred_element_type=jnp.float32)
        acts.append(activate(gate, linear))
    span = width // n_tp // 2
    for quarter in range(n_tp):
        for piece in range(2):
            start = (2 * quarter + piece) * span
            total = jnp.zeros((seqs, span), jnp.float32)
            for index, act in enumerate(acts):
                part = jnp.dot(
                    act,
                    down_ref[index, :, start : start + span],
                    preferred_element_type=jnp.float32,
                )
                total = total + part * wt_ref[:, index : index + 1]
            total = total.astype(jnp.bfloat16)
            for e in range(n_ep):
                out_ref[piece, e, quarter] = total[e * seq_dev : (e + 1) * seq_dev]


def run_experts(blocks, ffn_gain, w_gate, w_lin, w_down, own_weights, n_ep, n_tp, seq_dev):
    width = ffn_gain.shape[0]
    vmem = pl.BlockSpec(memory_space=pltpu.VMEM)
    return pl.pallas_call(
        functools.partial(expert_kernel, n_ep, n_tp),
        out_shape=(
            jax.ShapeDtypeStruct((2, n_ep, n_tp, seq_dev, width // n_tp // 2), jnp.bfloat16),
            jax.ShapeDtypeStruct((seq_dev, width), jnp.bfloat16),
        ),
        in_specs=[vmem] * 6,
        out_specs=(vmem, vmem),
        scratch_shapes=[pltpu.VMEM((n_ep * seq_dev, width), jnp.bfloat16)],
        compiler_params=pltpu.CompilerParams(vmem_limit_bytes=32 * 1024 * 1024),
    )(blocks, ffn_gain.reshape(1, -1), w_gate, w_lin, w_down, own_weights)


def on_device_dense(
    tokens,
    norm_gain,
    w_query,
    w_key,
    w_value,
    w_rgate,
    w_decay,
    decay_shift,
    state,
    head_gain,
    w_out,
    ffn_gain,
    w_gate,
    w_lin,
    w_down,
    expert_ids,
    route_weight,
):
    n_ep, n_tp = lax.axis_size("ep"), lax.axis_size("tp")
    my_ep, my_tp = lax.axis_index("ep"), lax.axis_index("tp")
    seq_dev, width = tokens.shape
    exp_dev = w_gate.shape[0]
    experts = exp_dev * n_ep
    seqs = seq_dev * n_ep
    span = width // n_ep
    lanes = -(-experts // 128) * 128
    named = expert_ids[:, :, None] == jnp.arange(lanes, dtype=jnp.int32)
    weights = jnp.sum(jnp.where(named, route_weight[:, :, None], 0.0), axis=1)

    rows, all_weights = spread_tokens(tokens, weights, n_ep)
    rows = rows.reshape(seqs, span)
    gain = lax.dynamic_slice_in_dim(norm_gain, my_ep * span, span).astype(jnp.float32)
    scaled = (rows.astype(jnp.float32) * gain).astype(jnp.bfloat16)
    parts = [
        jnp.dot(scaled, w, preferred_element_type=jnp.float32).astype(jnp.bfloat16)
        for w in (w_query, w_key, w_decay, w_value, w_rgate)
    ]
    joined = jnp.concatenate(parts, axis=1)
    sums = swap(joined.reshape(n_ep, seq_dev, -1), n_ep, False, 2)
    gated = gated_read(tokens, sums, decay_shift, state, head_gain)

    all_gated = swap(gated, n_ep, True, 3).reshape(seqs, -1)
    cols = w_out.shape[1] // n_tp
    partial_value = jnp.stack(
        [
            jnp.dot(
                all_gated, w_out[:, t * cols : (t + 1) * cols], preferred_element_type=jnp.float32
            ).astype(jnp.bfloat16)
            for t in range(n_tp)
        ]
    )
    own_tokens = lax.dynamic_slice_in_dim(rows, my_tp * cols, cols, axis=1)
    blocks = gather_stream(partial_value, own_tokens, n_ep, n_tp, 4)
    blocks = blocks.reshape(2, n_ep * n_tp, seqs // 2, cols)
    own_weights = lax.dynamic_slice_in_dim(
        all_weights.reshape(seqs, lanes), my_ep * exp_dev, exp_dev, axis=1
    )
    total, own_stream = run_experts(
        blocks, ffn_gain, w_gate, w_lin, w_down, own_weights, n_ep, n_tp, seq_dev
    )
    digits = (2,) * len(axes_of(n_ep, n_tp))
    routed = combine(total.reshape((2,) + digits + total.shape[-2:]), n_ep, n_tp, 5)
    routed = jnp.concatenate([routed[t, h] for t in range(n_tp) for h in range(2)], axis=1)
    return (own_stream.astype(jnp.float32) + routed.astype(jnp.float32)).astype(jnp.bfloat16)


def is_power(n):
    return n > 1 and n & (n - 1) == 0


def on_device(
    tokens,
    norm_gain,
    w_query,
    w_key,
    w_value,
    w_rgate,
    w_decay,
    decay_shift,
    state,
    head_gain,
    w_out,
    ffn_gain,
    w_gate,
    w_lin,
    w_down,
    expert_ids,
    route_weight,
):
    seq_dev = tokens.shape[0]
    width = tokens.shape[1]
    heads_dev = state.shape[1]
    key_dim = state.shape[2]
    val_dim = state.shape[3]
    key_cols = w_query.shape[1]
    val_cols = w_value.shape[1]
    inputs = tokens.astype(jnp.float32)
    normed = rms_scale(inputs, norm_gain.astype(jnp.float32)).astype(jnp.bfloat16)
    spread = lax.all_to_all(normed, "ep", split_axis=1, concat_axis=0, tiled=True)
    joined = jnp.concatenate((w_query, w_key, w_decay, w_value, w_rgate), axis=1)
    projected = lax.psum_scatter(
        jnp.dot(spread, joined, preferred_element_type=jnp.float32),
        "ep",
        scatter_dimension=0,
        tiled=True,
    )
    projected = projected.astype(jnp.bfloat16).astype(jnp.float32)
    q_rows = projected[:, :key_cols].reshape(seq_dev, heads_dev, key_dim) * key_dim ** (-0.5)
    k_rows = projected[:, key_cols : 2 * key_cols].reshape(seq_dev, heads_dev, key_dim)
    decay_pre = projected[:, 2 * key_cols : 3 * key_cols]
    v_rows = projected[:, 3 * key_cols : 3 * key_cols + val_cols].reshape(
        seq_dev, heads_dev, val_dim
    )
    rgates = projected[:, 3 * key_cols + val_cols :].reshape(seq_dev, heads_dev, val_dim)
    log_decay = jax.nn.log_sigmoid(decay_pre) / tau + decay_shift
    new_state = (
        jnp.exp(log_decay.reshape(seq_dev, heads_dev, key_dim))[..., None] * state
        + k_rows[..., None] * v_rows[:, :, None, :]
    )
    read = jnp.einsum("shk,shkv->shv", q_rows, new_state, precision=lax.Precision.HIGHEST)
    gated = rms_scale(
        read, head_gain.astype(jnp.float32).reshape(heads_dev, val_dim)
    ) * jax.nn.silu(rgates)
    gated = gated.reshape(seq_dev, heads_dev * val_dim).astype(jnp.bfloat16)
    partial_value = jnp.dot(
        lax.all_gather(gated, "ep", axis=0, tiled=True), w_out, preferred_element_type=jnp.float32
    )
    summed = lax.psum(partial_value.astype(jnp.bfloat16), "tp")
    mixed = lax.all_to_all(summed, "ep", split_axis=0, concat_axis=1, tiled=True)
    stream = inputs + mixed.astype(jnp.float32)
    ffn_in = rms_scale(stream, ffn_gain.astype(jnp.float32)).astype(jnp.bfloat16)
    n_ep = lax.axis_size("ep")
    exp_dev = w_gate.shape[0]
    experts = exp_dev * n_ep
    top = expert_ids.shape[1]
    capacity = max(2, 2 * seq_dev * top // experts)
    flat_ids = expert_ids.reshape(-1)
    onehot = (flat_ids[:, None] == jnp.arange(experts, dtype=jnp.int32)[None, :]).astype(jnp.int32)
    rank = jnp.sum((jnp.cumsum(onehot, axis=0) - onehot) * onehot, axis=1)
    slot_of = flat_ids * capacity + rank
    dispatch = (
        jnp.arange(experts * capacity, dtype=jnp.int32)[:, None] == slot_of[None, :]
    ).astype(jnp.bfloat16)
    dispatch = jnp.sum(dispatch.reshape(experts * capacity, seq_dev, top), axis=2)
    outbound = jnp.dot(dispatch, ffn_in, preferred_element_type=jnp.float32).astype(jnp.bfloat16)
    outbound = outbound.reshape(experts, capacity, width)
    arrived = lax.all_to_all(outbound, "ep", split_axis=0, concat_axis=0, tiled=True)
    count = arrived.shape[1]
    rows = arrived.reshape(n_ep, exp_dev, count, width)
    gate = jnp.einsum("secd,edh->sech", rows, w_gate, preferred_element_type=jnp.float32)
    linear = jnp.einsum("secd,edh->sech", rows, w_lin, preferred_element_type=jnp.float32)
    act = activate(gate, linear)
    partial_out = jnp.einsum("sech,ehd->secd", act, w_down, preferred_element_type=jnp.float32)
    summed_out = lax.psum(partial_out.astype(jnp.bfloat16), "tp")
    returned = lax.all_to_all(
        summed_out.reshape(n_ep * exp_dev, count, width),
        "ep",
        split_axis=0,
        concat_axis=0,
        tiled=True,
    )
    picked = (
        returned.reshape(experts * capacity, width)[slot_of]
        .astype(jnp.float32)
        .reshape(seq_dev, top, width)
    )
    routed = jnp.sum(picked * route_weight[..., None], axis=1)
    return (stream + routed).astype(jnp.bfloat16)


def solution(mesh):
    n_ep, n_tp = mesh.shape["ep"], mesh.shape["tp"]

    def chosen(*arrays):
        seq_dev, top = arrays[15].shape
        experts = arrays[12].shape[0] * n_ep
        dense = max(2, 2 * seq_dev * top // experts) >= seq_dev
        whole = arrays[0].shape[1] % (n_ep * n_tp * 128) == 0 and seq_dev % 8 == 0
        if dense and whole and is_power(n_ep) and is_power(n_tp):
            return on_device_dense(*arrays)
        return on_device(*arrays)

    placed = (
        P("ep", None),
        P(),
        P("ep", "tp"),
        P("ep", "tp"),
        P("ep", "tp"),
        P("ep", "tp"),
        P("ep", "tp"),
        P("ep", "tp"),
        P("ep", "tp", None, None),
        P("tp"),
        P("tp", "ep"),
        P(),
        P("ep", None, "tp"),
        P("ep", None, "tp"),
        P("ep", "tp", None),
        P("ep", None),
        P("ep", None),
    )
    return jax.shard_map(
        chosen, mesh=mesh, in_specs=placed, out_specs=P("ep", None), check_vma=False
    )
```
